512 devices in a mesh: ep: 32 (over z, core), tp: 16 (over y, x).
Axes of the slice: x: 4, y: 4, z: 16, core: 2. Of those that a mesh axis runs over, the one named last changes fastest.
Arguments:
- queries: bfloat16 [8192, 2048], P('ep', 'tp'), may hold values from -6 to 6
- key_rows: bfloat16 [8192, 1024], P('ep', 'tp'), may hold values from -6 to 6
- values: bfloat16 [8192, 1024], P('ep', 'tp'), may hold values from -140 to 140
- query_gain: float32 [64], replicated, may hold values from 0.55 to 7.5
- key_gain: float32 [64], replicated, may hold values from 0.55 to 7.5
- mix_gain: float32 [2048], replicated, may hold values from 0.1 to 1.9
- out_weight: bfloat16 [2048, 4096], P(None, 'tp'), may hold values from -0.125 to 0.125
- expert_input: bfloat16 [8192, 4096], P('ep', 'tp'), may hold values from -140 to 140
- expert_gain: float32 [4096], replicated, may hold values from 0.1 to 1.9
- route_ids: int32 [8192, 2], P('ep'), may hold values from 0 to 31, as said below
- route_weights: float32 [8192, 2], P('ep'), may hold values from 0.3 to 1.7
- expert_gate: bfloat16 [32, 4096, 2048], P('ep', None, 'tp'), may hold values from -0.09375 to 0.09375
- expert_up: bfloat16 [32, 4096, 2048], P('ep', None, 'tp'), may hold values from -0.09375 to 0.09375
- expert_down: bfloat16 [32, 2048, 4096], P('ep', None, 'tp'), may hold values from -0.125 to 0.125
Outputs:
- attended: bfloat16 [8192, 4096], P('ep', 'tp')
- expert_mix: bfloat16 [8192, 4096], P('ep', 'tp')
The draws below stay inside these ranges and needn't reach their ends.
Inputs may be any that keep to these rules, and one draw needn't show every extreme that they name: `route_ids`: the 2 experts of a row differ. In every aligned block of 256 rows no expert is named more than 22 times, and one expert, the same for all blocks, is named exactly 22 times in every block.
All inputs are finite; a program needn't handle non-finite values.
Results may differ from the reference program's by a relative error of at most 0.01.
The reference program's roundings to bfloat16 on the way count: a program that leaves them out, or rounds other values in their place, can miss the bound.
Values may be sent and summed in bfloat16 or wider, within the bound.
No kernel may reach another device: no remote copies, remote signals or barrier semaphores. Data moves between devices by JAX's collectives and lax.ppermute only.
A program may use at most 64 MiB of HBM per device.

```python
import math
import jax
import jax.numpy as jnp
from jax import lax

D = 4096
Q_HEADS = 32
KV_HEADS = 16
HEAD = 64
FF = 2048
TOP_K = 2
GRID_W = 64
TOK_DEV = 256
TOKENS = 8192
EXPERTS = 32
CAP = 22
N_EP = 32


def draw_key_rows(key, part):
    field_data = jnp.clip(jax.random.normal(jax.random.fold_in(key, 7), (TOKENS, KV_HEADS * HEAD), jnp.float32), -6.0, 6.0)
    return field_data.astype(jnp.bfloat16)


def draw_queries(key, part):
    field_data = jnp.clip(jax.random.normal(jax.random.fold_in(key, 9), (TOKENS, Q_HEADS * HEAD), jnp.float32), -6.0, 6.0)
    return field_data.astype(jnp.bfloat16)


def rising_field(seed_key, row_count, column_count, group_width):
    pieces = jax.random.split(seed_key, 2)
    group_count = column_count // group_width
    position = (jnp.arange(column_count) // group_width).astype(jnp.float32) / max(group_count - 1, 1)
    jitter = jax.random.uniform(pieces[1], (column_count,), jnp.float32)
    log_scale = math.log(10.0) * 0.5 * (position + jitter)
    field_data = jnp.clip(jax.random.normal(pieces[0], (row_count, column_count), jnp.float32), -4.0, 4.0)
    return field_data * jnp.exp(log_scale)


def draw_values(key, part):
    return rising_field(jax.random.fold_in(key, 3), TOKENS, KV_HEADS * HEAD, HEAD).astype(jnp.bfloat16)


def draw_expert_input(key, part):
    return rising_field(jax.random.fold_in(key, 5), TOKENS, D, 1).astype(jnp.bfloat16)


def draw_query_gain(key, part):
    seed_key = jax.random.fold_in(key, 21)
    return jax.random.uniform(seed_key, (HEAD,), jnp.float32, 0.55, 1.45)


def draw_key_gain(key, part):
    seed_key = jax.random.fold_in(key, 23)
    return jax.random.uniform(seed_key, (HEAD,), jnp.float32, 0.55, 1.45)


def block_routes(seed_key, favored):
    ticket_total = TOK_DEV * TOP_K
    pieces = jax.random.split(seed_key, 3)
    ticket_order = jax.random.permutation(pieces[0], (EXPERTS - 1) * CAP)
    live_slots = (ticket_order < ticket_total - CAP).astype(jnp.int32).reshape(EXPERTS - 1, CAP)
    rest_counts = jnp.sum(live_slots, axis=1).astype(jnp.int32)
    everyone = jnp.arange(EXPERTS, dtype=jnp.int32)
    rest_index = jnp.clip(everyone - (everyone > favored).astype(jnp.int32), 0, max(EXPERTS - 2, 0))
    counts = jnp.where(everyone == favored, CAP, rest_counts[rest_index]).astype(jnp.int32)
    run_order = jax.random.permutation(pieces[1], EXPERTS).astype(jnp.int32)
    run_ends = jnp.cumsum(counts[run_order]).astype(jnp.int32)
    run_index = jnp.searchsorted(run_ends, jnp.arange(ticket_total, dtype=jnp.int32), side='right')
    tickets = run_order[run_index]
    by_row = tickets.reshape(TOP_K, TOK_DEV).T
    row_order = jax.random.permutation(pieces[2], TOK_DEV)
    return jnp.zeros((TOK_DEV, TOP_K), jnp.int32).at[row_order].set(by_row)


def draw_route_ids(key, part):
    base_key = jax.random.fold_in(key, 13)
    favored = jax.random.randint(jax.random.fold_in(base_key, 1), (), 0, EXPERTS).astype(jnp.int32)
    block_keys = jax.random.split(jax.random.fold_in(base_key, 2), N_EP)
    routes = jax.vmap(block_routes, in_axes=(0, None))(block_keys, favored)
    return routes.reshape(TOKENS, TOP_K).astype(jnp.int32)


def steps_of(key, extent, shards, least, high):
    def one(dim, parts):
        draws = jax.random.uniform(jax.random.fold_in(jax.random.fold_in(key, 6), dim), (parts,), jnp.float32, least / len(shards), high / len(shards))
        return jnp.repeat(jnp.exp(draws), extent[dim] // parts).reshape((-1,) + (1,) * (len(extent) - dim - 1))

    gain = one(*shards[0])
    for cut in shards[1:]:
        gain = gain * one(*cut)
    return gain


def scatter_about(own_key, dims, spread, limit, cuts=(), held_as=jnp.bfloat16):
    loudness = steps_of(own_key, dims, cuts, -0.22, 0.18) if cuts else 1.0
    result = jax.random.normal(own_key, dims, jnp.float32) * spread * loudness
    return jnp.minimum(jnp.maximum(result, -limit), limit).astype(held_as)


def setup_inputs(seed: int = 0) -> dict:
    key_of = jax.random.split(jax.random.key(seed), 15)
    queries = draw_queries(jax.random.fold_in(key_of[14], 71), 0)
    key_rows = draw_key_rows(jax.random.fold_in(key_of[14], 71), 0)
    values = draw_values(jax.random.fold_in(key_of[14], 71), 0)
    query_gain = draw_query_gain(jax.random.fold_in(key_of[14], 71), 0)
    key_gain = draw_key_gain(jax.random.fold_in(key_of[14], 71), 0)
    mix_gain = jnp.clip(1.0 + 0.18 * jax.random.normal(key_of[5], (Q_HEADS * HEAD,), jnp.float32), 0.1, 1.9)
    out_weight = scatter_about(key_of[6], (Q_HEADS * HEAD, D), (Q_HEADS * HEAD) ** -0.5, 0.125, ((1, 16),))
    expert_input = draw_expert_input(jax.random.fold_in(key_of[14], 71), 0)
    expert_gain = jnp.clip(1.0 + 0.18 * jax.random.normal(key_of[8], (D,), jnp.float32), 0.1, 1.9)
    route_ids = draw_route_ids(jax.random.fold_in(key_of[14], 71), 0)
    route_weights = jnp.clip(0.3 + 1.40000004 * jax.random.uniform(key_of[10], (TOKENS, TOP_K), jnp.float32) ** steps_of(key_of[10], (TOKENS, TOP_K), ((0, 32),), -0.2, 0.2), 0.3, 1.7)
    expert_gate = scatter_about(key_of[11], (EXPERTS, D, FF), D ** -0.5, 0.09375, ((0, 32), (2, 16)))
    expert_up = scatter_about(key_of[12], (EXPERTS, D, FF), D ** -0.5, 0.09375, ((0, 32), (2, 16)))
    expert_down = scatter_about(key_of[13], (EXPERTS, FF, D), FF ** -0.5, 0.125, ((0, 32), (2, 16)))
    return dict(queries=queries, key_rows=key_rows, values=values, query_gain=query_gain, key_gain=key_gain, mix_gain=mix_gain, out_weight=out_weight, expert_input=expert_input, expert_gain=expert_gain, route_ids=route_ids, route_weights=route_weights, expert_gate=expert_gate, expert_up=expert_up, expert_down=expert_down)


EPS = 1e-06
THETA = 10000.0

def turn_tables(length):
    half_width = HEAD // 2
    inverse = THETA ** (-jnp.arange(0, half_width, 2, dtype=jnp.float32) / half_width)
    positions = jnp.arange(length, dtype=jnp.int32)
    grid_rows = (positions // GRID_W).astype(jnp.float32)
    grid_cols = (positions % GRID_W).astype(jnp.float32)
    angles = jnp.concatenate([grid_rows[:, None] * inverse, grid_cols[:, None] * inverse], axis=-1)
    return (jnp.cos(angles), jnp.sin(angles))

def norm_turn(source, scale_gain, cosine_table, sine_table):
    length = source.shape[0]
    head_rows = source.astype(jnp.float32).reshape(length, -1, HEAD)
    head_rows = head_rows * lax.rsqrt(lax.optimization_barrier(jnp.mean(head_rows * head_rows, axis=-1, keepdims=True)) + EPS) * scale_gain
    pair_view = head_rows.reshape(length, head_rows.shape[1], HEAD // 2, 2)
    even_part = pair_view[..., 0]
    odd_part = pair_view[..., 1]
    cosine_part = cosine_table[:, None, :]
    sine_part = sine_table[:, None, :]
    turned = jnp.stack([even_part * cosine_part - odd_part * sine_part, even_part * sine_part + odd_part * cosine_part], axis=-1)
    return turned.reshape(length, -1).astype(jnp.bfloat16)

def attend_head(operands):
    query_group, key_head, value_head = operands
    length = query_group.shape[0]
    block_rows = math.gcd(length, 512)
    query_blocks = query_group.reshape(length // block_rows, block_rows, query_group.shape[1], HEAD)
    keys_float = key_head.astype(jnp.float32)
    values_float = value_head.astype(jnp.float32)

    def one_block(query_block):
        scores = jnp.einsum('rgd,nd->grn', query_block.astype(jnp.float32), keys_float) / math.sqrt(HEAD)
        row_max = lax.optimization_barrier(jnp.max(scores, axis=-1, keepdims=True))
        raw_weights = jnp.exp(scores - row_max)
        row_total = lax.optimization_barrier(jnp.sum(raw_weights, axis=-1))
        rounded = lax.optimization_barrier(raw_weights.astype(jnp.bfloat16)).astype(jnp.float32)
        summed = jnp.einsum('grn,nd->rgd', rounded, values_float)
        return (summed / jnp.transpose(row_total)[:, :, None]).astype(jnp.bfloat16)
    return lax.map(one_block, query_blocks).reshape(length, -1)

def reference(queries, key_rows, values, query_gain, key_gain, mix_gain, out_weight, expert_input, expert_gain, route_ids, route_weights, expert_gate, expert_up, expert_down):
    length = queries.shape[0]
    cosine_table, sine_table = turn_tables(length)
    query_turned = norm_turn(queries, query_gain, cosine_table, sine_table)
    key_turned = norm_turn(key_rows, key_gain, cosine_table, sine_table)
    group_size = Q_HEADS // KV_HEADS
    query_heads = query_turned.reshape(length, KV_HEADS, group_size, HEAD).transpose(1, 0, 2, 3)
    key_heads = key_turned.reshape(length, KV_HEADS, HEAD).transpose(1, 0, 2)
    value_heads = values.reshape(length, KV_HEADS, HEAD).transpose(1, 0, 2)
    heads_out = lax.map(attend_head, (query_heads, key_heads, value_heads))
    heads_out = heads_out.transpose(1, 0, 2).reshape(length, Q_HEADS * HEAD)
    heads_float = heads_out.astype(jnp.float32)
    mix_scale = lax.rsqrt(lax.optimization_barrier(jnp.mean(heads_float * heads_float, axis=-1)) + EPS)
    mix_in = (heads_float * mix_gain).astype(jnp.bfloat16)
    attended = (jnp.dot(mix_in, out_weight, preferred_element_type=jnp.float32) * mix_scale[:, None]).astype(jnp.bfloat16)
    blocks = N_EP
    copies = TOK_DEV * TOP_K
    ids_block = route_ids.reshape(blocks, copies).astype(jnp.int32)
    hit_marks = (ids_block[:, :, None] == jnp.arange(EXPERTS, dtype=jnp.int32)[None, None, :]).astype(jnp.int32)
    earlier = (jnp.cumsum(hit_marks, axis=1) - hit_marks).astype(jnp.int32)
    places = lax.optimization_barrier(jnp.sum(earlier * hit_marks, axis=2)).astype(jnp.int32)
    block_index = jnp.broadcast_to(jnp.arange(blocks, dtype=jnp.int32)[:, None], (blocks, copies))
    token_index = block_index * TOK_DEV + (jnp.arange(copies, dtype=jnp.int32) // TOP_K)[None, :]
    slot_table = jnp.full((EXPERTS, blocks, CAP), length, jnp.int32)
    slot_table = slot_table.at[ids_block, block_index, places].set(token_index.astype(jnp.int32))
    input_float = expert_input.astype(jnp.float32)
    expert_stat = lax.rsqrt(lax.optimization_barrier(jnp.mean(input_float * input_float, axis=-1)) + EPS)
    expert_scaled = (input_float * expert_gain).astype(jnp.bfloat16)
    scaled_pad = jnp.concatenate([expert_scaled, jnp.zeros((1, D), jnp.bfloat16)], axis=0)
    stat_pad = jnp.concatenate([expert_stat, jnp.zeros((1,), jnp.float32)], axis=0)

    def run_expert(operands):
        slot_tokens, gate_weight, up_weight, down_weight = operands
        flat_tokens = slot_tokens.reshape(-1)
        slot_input = scaled_pad[flat_tokens]
        row_stat = stat_pad[flat_tokens][:, None]
        gate_value = jnp.dot(slot_input, gate_weight, preferred_element_type=jnp.float32) * row_stat
        up_value = jnp.dot(slot_input, up_weight, preferred_element_type=jnp.float32) * row_stat
        hidden = (jax.nn.silu(gate_value) * up_value).astype(jnp.bfloat16)
        return jnp.dot(hidden, down_weight, preferred_element_type=jnp.float32).astype(jnp.bfloat16)
    outputs = lax.map(run_expert, (slot_table, expert_gate, expert_up, expert_down))
    picked = outputs[ids_block, block_index * CAP + places].astype(jnp.float32)
    weighted = picked * route_weights.reshape(blocks, copies)[:, :, None]
    expert_mix = lax.optimization_barrier(jnp.sum(weighted.reshape(length, TOP_K, D), axis=1)).astype(jnp.bfloat16)
    return (attended, expert_mix)
```

```python
import jax
import jax.numpy as jnp
from jax import lax
from jax.experimental import pallas as pl
from jax.experimental.pallas import tpu as pltpu
from jax.sharding import Mesh
from jax.sharding import PartitionSpec as P


HEAD = 64
GRID_W = 64
EPS = 1e-06
THETA = 10000.0
EP = ("z", "c")
TP = ("y", "x")
SIDE = 4
CAP = 22
KEY_STEP = 2048

F32 = jnp.float32
BF16 = jnp.bfloat16


def turn_tables(offset, length):
    half_width = HEAD // 2
    inverse = THETA ** (-jnp.arange(0, half_width, 2, dtype=F32) / half_width)
    positions = offset + jnp.arange(length, dtype=jnp.int32)
    grid_rows = (positions // GRID_W).astype(F32)
    grid_cols = (positions % GRID_W).astype(F32)
    angles = jnp.concatenate([grid_rows[:, None] * inverse, grid_cols[:, None] * inverse], axis=-1)
    return (jnp.cos(angles), jnp.sin(angles))


def norm_turn(source, scale_gain, cosine_table, sine_table):
    length = source.shape[0]
    head_rows = source.astype(F32).reshape(length, -1, HEAD)
    head_rows = (
        head_rows
        * lax.rsqrt(jnp.mean(head_rows * head_rows, axis=-1, keepdims=True) + EPS)
        * scale_gain
    )
    pair_view = head_rows.reshape(length, head_rows.shape[1], HEAD // 2, 2)
    even_part = pair_view[..., 0]
    odd_part = pair_view[..., 1]
    cosine_part = cosine_table[:, None, :]
    sine_part = sine_table[:, None, :]
    turned = jnp.stack(
        [
            even_part * cosine_part - odd_part * sine_part,
            even_part * sine_part + odd_part * cosine_part,
        ],
        axis=-1,
    )
    return turned.reshape(length, -1).astype(BF16)


def attend_body(q_ref, mine_ref, other_ref, out_ref):
    rows = q_ref.shape[0]
    lanes = lax.broadcasted_iota(jnp.int32, (rows, 2 * HEAD), 1)
    both = q_ref[...].astype(F32)
    low = jnp.where(lanes < HEAD, both, 0.0)
    high = pltpu.roll(jnp.where(lanes < HEAD, 0.0, both), HEAD, 1)
    wide = (jnp.concatenate([low, high], axis=0) * 0.125).astype(BF16)
    top = jnp.full((2 * rows, 1), -jnp.inf, F32)
    total = jnp.zeros((2 * rows, 1), F32)
    acc = jnp.zeros((2 * rows, 2 * HEAD), F32)
    steps = [
        (ref, at) for ref in (mine_ref, other_ref) for at in range(0, ref.shape[0], KEY_STEP)
    ]
    for ref, at in steps:
        block = ref[at : at + KEY_STEP, :]
        scores = lax.dot_general(wide, block, (((1,), (1,)), ((), ())), preferred_element_type=F32)
        new_top = jnp.maximum(top, jnp.max(scores, axis=1, keepdims=True))
        factor = jnp.exp(top - new_top)
        raw = jnp.exp(scores - new_top)
        total = total * factor + jnp.sum(raw, axis=1, keepdims=True)
        acc = acc * factor + jnp.dot(raw.astype(BF16), block, preferred_element_type=F32)
        top = new_top
    done = acc / total
    first = pltpu.roll(done[:rows], HEAD, 1)
    out_ref[...] = jnp.where(lanes < HEAD, first, done[rows:]).astype(BF16)


def attend(query_turned, mine, other):
    rows = query_turned.shape[0]
    keys = mine.shape[0] + other.shape[0]
    return pl.pallas_call(
        attend_body,
        out_shape=jax.ShapeDtypeStruct(query_turned.shape, BF16),
        compiler_params=pltpu.CompilerParams(vmem_limit_bytes=48 * 1024 * 1024),
        cost_estimate=pl.CostEstimate(
            flops=16 * rows * keys * HEAD,
            bytes_accessed=keys * 4 * HEAD,
            transcendentals=2 * rows * keys,
        ),
        name="attend",
    )(query_turned, mine, other)


def two_parts(value):
    high = lax.reduce_precision(value, 8, 7)
    return high.astype(BF16), (value - high).astype(BF16)


def stat_rows(sums, count):
    width = 256
    flat = jnp.pad(sums, (0, count * width - sums.shape[0])).reshape(count, width)
    high, low = two_parts(flat)
    return jnp.concatenate([high, low], axis=0)


def read_stat(rows, count, size):
    whole = rows.astype(F32)
    return jnp.sum(whole[:, :count] + whole[:, count:], axis=0).reshape(-1)[:size]


def copies_to(array, axis):
    wide = jnp.broadcast_to(array[None], (SIDE,) + array.shape)
    return lax.all_to_all(wide, axis, 0, 0, tiled=True)


def swap(array, axis):
    return lax.all_to_all(array, axis, 0, 0, tiled=True)


def shift(array, axis, by):
    size = lax.axis_size(axis)
    return lax.ppermute(array, axis, [(k, (k + by) % size) for k in range(size)])


def keys_everywhere(block):
    far = [block] + [shift(block, "z", by) for by in (4, 12, 8)]
    strided = jnp.concatenate(far, axis=0)
    near = [strided] + [shift(strided, "z", by) for by in (1, 15, 2)]
    mine = jnp.concatenate(near, axis=0)
    return mine, shift(mine, "c", 1)


def deal(chunk_for, axis):
    place = lax.axis_index(axis)
    landed = [chunk_for(place)]
    for by in range(1, SIDE):
        landed.append(shift(chunk_for((place + by) % SIDE), axis, by))
    return in_order(jnp.stack(landed), place)


def in_order(landed, place):
    return jnp.stack(
        [
            lax.dynamic_index_in_dim(landed, (place - k) % SIDE, 0, keepdims=False)
            for k in range(SIDE)
        ]
    )


def forward(
    queries,
    key_rows,
    values,
    query_gain,
    key_gain,
    mix_gain,
    out_weight,
    expert_input,
    expert_gain,
    route_ids,
    route_weights,
    expert_gate,
    expert_up,
    expert_down,
):
    length = queries.shape[0]
    experts_count = lax.axis_size(EP)
    place_x = lax.axis_index("x")
    place_y = lax.axis_index("y")
    slot_total = experts_count * CAP
    features = expert_gain.shape[0]
    piece = expert_input.shape[1]
    hid = expert_gate.shape[2]

    cosine_table, sine_table = turn_tables(lax.axis_index(EP) * length, length)
    key_turned = norm_turn(key_rows, key_gain, cosine_table, sine_table)
    mine, other = keys_everywhere(jnp.concatenate([key_turned, values], axis=1))
    query_turned = norm_turn(queries, query_gain, cosine_table, sine_table)

    copies = length * 2
    flat_ids = route_ids.reshape(copies)
    hit_marks = (flat_ids[:, None] == jnp.arange(experts_count, dtype=jnp.int32)[None, :]).astype(
        jnp.int32
    )
    earlier = jnp.cumsum(hit_marks, axis=0) - hit_marks
    places = jnp.sum(earlier * hit_marks, axis=1)
    slot_index = (flat_ids * CAP + places).reshape(length, 2)
    slot_axis = jnp.arange(slot_total, dtype=jnp.int32)
    pick = (
        (slot_index[:, 0][None, :] == slot_axis[:, None])
        | (slot_index[:, 1][None, :] == slot_axis[:, None])
    ).astype(BF16)
    outgoing = jnp.dot(pick, expert_input, preferred_element_type=F32).astype(BF16)
    arrived = swap(outgoing.reshape(experts_count, CAP, piece), EP).reshape(slot_total, piece)

    gate_view = expert_gate.reshape(SIDE, SIDE, piece, hid)
    up_view = expert_up.reshape(SIDE, SIDE, piece, hid)

    def first_chunk(k):
        pair = [lax.dynamic_index_in_dim(w, k, 1, keepdims=False) for w in (gate_view, up_view)]
        return jnp.concatenate(pair, axis=2).reshape(SIDE * piece, 2 * hid)

    def second_chunk(k):
        down = lax.dynamic_slice_in_dim(expert_down[0], k * SIDE * hid, SIDE * hid, 0)
        out = lax.dynamic_slice_in_dim(out_weight, k * SIDE * 2 * HEAD, SIDE * 2 * HEAD, 0)
        return jnp.concatenate([down, out], axis=0)

    first_weights = deal(first_chunk, "x")
    second_weights = deal(second_chunk, "y")

    gathered = copies_to(arrived, "y")
    gains = lax.dynamic_index_in_dim(
        expert_gain.reshape(SIDE, SIDE, piece), place_x, axis=1, keepdims=False
    )
    gathered_float = gathered.astype(F32)
    scaled = (gathered_float * gains[:, None, :]).astype(BF16)
    squares = jnp.sum(gathered_float * gathered_float, axis=(0, 2))
    partial = jnp.einsum(
        "ysf,xyfh->xsh",
        scaled,
        first_weights.reshape(SIDE, SIDE, piece, 2 * hid),
        preferred_element_type=F32,
    ).astype(BF16)
    stat_count = -(-slot_total // piece)
    stats = jnp.broadcast_to(stat_rows(squares, stat_count)[None], (SIDE, 2 * stat_count, piece))
    received = swap(jnp.concatenate([partial, stats], axis=1), "x")
    sums = jnp.sum(received[:, :slot_total].astype(F32), axis=0)
    square_sum = read_stat(received[:, slot_total:], stat_count, slot_total)
    row_stat = lax.rsqrt(square_sum / features + EPS)
    gate_value = sums[:, :hid] * row_stat[:, None]
    up_value = sums[:, hid:] * row_stat[:, None]
    hidden = (jax.nn.silu(gate_value) * up_value).astype(BF16)

    hidden_all = copies_to(hidden, "x")
    down_rows = second_weights[:, : SIDE * hid].reshape(SIDE, SIDE, hid, piece)
    out_rows = second_weights[:, SIDE * hid :].reshape(SIDE, SIDE, 2 * HEAD, piece)
    expert_partial = jnp.einsum(
        "xsh,yxhf->ysf", hidden_all, down_rows, preferred_element_type=F32
    ).astype(BF16)
    landed = swap(expert_partial, "y")
    expert_out = jnp.sum(landed.astype(F32), axis=0).astype(BF16)

    heads_out = attend(query_turned, mine, other)
    near = jnp.stack([heads_out] + [shift(heads_out, "x", by) for by in range(1, SIDE)])
    heads = in_order(near, place_x)
    head_float = heads.astype(F32)
    mix_gains = lax.dynamic_index_in_dim(
        mix_gain.reshape(SIDE, SIDE, 2 * HEAD), place_y, axis=0, keepdims=False
    )
    mix_in = (head_float * mix_gains[:, None, :]).astype(BF16)
    mix_squares = jnp.sum(head_float * head_float, axis=(0, 2))
    mix_partial = jnp.einsum(
        "xsh,yxhf->ysf", mix_in, out_rows, preferred_element_type=F32
    ).astype(BF16)
    mix_stats = jnp.broadcast_to(stat_rows(mix_squares, 1)[None], (SIDE, 2, piece))
    payload = jnp.concatenate([mix_partial, mix_stats], axis=1)

    def payload_of(k):
        return lax.dynamic_index_in_dim(payload, k, 0, keepdims=False)

    parts = [payload_of(place_y)] + [
        shift(payload_of((place_y + by) % SIDE), "y", by) for by in range(1, SIDE)
    ]
    mix_sum = sum(part[:length].astype(F32) for part in parts)
    mix_square_sum = read_stat(jnp.stack([part[length:] for part in parts]), 1, length)
    mix_scale = lax.rsqrt(mix_square_sum / mix_gain.shape[0] + EPS)
    attended = (mix_sum * mix_scale[:, None]).astype(BF16)

    returned = swap(expert_out.reshape(experts_count, CAP, piece), EP).reshape(slot_total, piece)
    slots = slot_axis[None, :]
    first = jnp.dot(
        (slot_index[:, :1] == slots).astype(BF16), returned, preferred_element_type=F32
    )
    second = jnp.dot(
        (slot_index[:, 1:] == slots).astype(BF16), returned, preferred_element_type=F32
    )
    expert_mix = (first * route_weights[:, :1] + second * route_weights[:, 1:]).astype(BF16)
    return (attended, expert_mix)


def solution(mesh):
    torus = Mesh(mesh.devices.reshape(-1, 2, SIDE, SIDE), ("z", "c", "y", "x"))
    return jax.shard_map(
        forward,
        mesh=torus,
        in_specs=(
            P(EP, TP),
            P(EP, TP),
            P(EP, TP),
            P(),
            P(),
            P(),
            P(None, TP),
            P(EP, TP),
            P(),
            P(EP, None),
            P(EP, None),
            P(EP, None, TP),
            P(EP, None, TP),
            P(EP, None, TP),
        ),
        out_specs=(P(EP, TP), P(EP, TP)),
        check_vma=False,
    )
```

```python
import jax
import jax.numpy as jnp
from jax import lax
from jax.experimental import pallas as pl
from jax.experimental.pallas import tpu as pltpu
from jax.sharding import Mesh
from jax.sharding import PartitionSpec as P


HEAD = 64
GRID_W = 64
EPS = 1e-06
THETA = 10000.0
EP = ("z", "c")
TP = ("y", "x")
SIDE = 4
CAP = 22
KEY_STEP = 2048

F32 = jnp.float32
BF16 = jnp.bfloat16


def turn_tables(offset, length):
    half_width = HEAD // 2
    inverse = THETA ** (-jnp.arange(0, half_width, 2, dtype=F32) / half_width)
    positions = offset + jnp.arange(length, dtype=jnp.int32)
    grid_rows = (positions // GRID_W).astype(F32)
    grid_cols = (positions % GRID_W).astype(F32)
    angles = jnp.concatenate([grid_rows[:, None] * inverse, grid_cols[:, None] * inverse], axis=-1)
    return (jnp.cos(angles), jnp.sin(angles))


def norm_turn(source, scale_gain, cosine_table, sine_table):
    length = source.shape[0]
    head_rows = source.astype(F32).reshape(length, -1, HEAD)
    head_rows = (
        head_rows
        * lax.rsqrt(jnp.mean(head_rows * head_rows, axis=-1, keepdims=True) + EPS)
        * scale_gain
    )
    pair_view = head_rows.reshape(length, head_rows.shape[1], HEAD // 2, 2)
    even_part = pair_view[..., 0]
    odd_part = pair_view[..., 1]
    cosine_part = cosine_table[:, None, :]
    sine_part = sine_table[:, None, :]
    turned = jnp.stack(
        [
            even_part * cosine_part - odd_part * sine_part,
            even_part * sine_part + odd_part * cosine_part,
        ],
        axis=-1,
    )
    return turned.reshape(length, -1).astype(BF16)


def attend_body(q_ref, kv_ref, out_ref):
    rows = q_ref.shape[0]
    lanes = lax.broadcasted_iota(jnp.int32, (rows, 2 * HEAD), 1)
    both = q_ref[...].astype(F32)
    low = jnp.where(lanes < HEAD, both, 0.0)
    high = pltpu.roll(jnp.where(lanes < HEAD, 0.0, both), HEAD, 1)
    wide = (jnp.concatenate([low, high], axis=0) * 0.125).astype(BF16)
    top = jnp.full((2 * rows, 1), -jnp.inf, F32)
    total = jnp.zeros((2 * rows, 1), F32)
    acc = jnp.zeros((2 * rows, 2 * HEAD), F32)
    for at in range(0, kv_ref.shape[0], KEY_STEP):
        block = kv_ref[at : at + KEY_STEP, :]
        scores = lax.dot_general(wide, block, (((1,), (1,)), ((), ())), preferred_element_type=F32)
        new_top = jnp.maximum(top, jnp.max(scores, axis=1, keepdims=True))
        factor = jnp.exp(top - new_top)
        raw = jnp.exp(scores - new_top)
        total = total * factor + jnp.sum(raw, axis=1, keepdims=True)
        acc = acc * factor + jnp.dot(raw.astype(BF16), block, preferred_element_type=F32)
        top = new_top
    done = acc / total
    first = pltpu.roll(done[:rows], HEAD, 1)
    out_ref[...] = jnp.where(lanes < HEAD, first, done[rows:]).astype(BF16)


def attend(query_turned, key_value):
    rows = query_turned.shape[0]
    keys = key_value.shape[0]
    return pl.pallas_call(
        attend_body,
        out_shape=jax.ShapeDtypeStruct(query_turned.shape, BF16),
        compiler_params=pltpu.CompilerParams(vmem_limit_bytes=48 * 1024 * 1024),
        cost_estimate=pl.CostEstimate(
            flops=16 * rows * keys * HEAD,
            bytes_accessed=keys * 4 * HEAD,
            transcendentals=2 * rows * keys,
        ),
        name="attend",
    )(query_turned, key_value)


def two_parts(value):
    high = lax.reduce_precision(value, 8, 7)
    return high.astype(BF16), (value - high).astype(BF16)


def stat_rows(sums, count):
    width = 256
    flat = jnp.pad(sums, (0, count * width - sums.shape[0])).reshape(count, width)
    high, low = two_parts(flat)
    return jnp.concatenate([high, low], axis=0)


def read_stat(rows, count, size):
    whole = rows.astype(F32)
    return jnp.sum(whole[:, :count] + whole[:, count:], axis=0).reshape(-1)[:size]


def copies_to(array, axis):
    wide = jnp.broadcast_to(array[None], (SIDE,) + array.shape)
    return lax.all_to_all(wide, axis, 0, 0, tiled=True)


def swap(array, axis):
    return lax.all_to_all(array, axis, 0, 0, tiled=True)


def shift(array, axis, by):
    size = lax.axis_size(axis)
    return lax.ppermute(array, axis, [(k, (k + by) % size) for k in range(size)])


def deal(chunk_for, axis):
    place = lax.axis_index(axis)
    landed = [chunk_for(place)]
    for by in range(1, SIDE):
        landed.append(shift(chunk_for((place + by) % SIDE), axis, by))
    return in_order(jnp.stack(landed), place)


def in_order(landed, place):
    return jnp.stack(
        [
            lax.dynamic_index_in_dim(landed, (place - k) % SIDE, 0, keepdims=False)
            for k in range(SIDE)
        ]
    )


def forward(
    queries,
    key_rows,
    values,
    query_gain,
    key_gain,
    mix_gain,
    out_weight,
    expert_input,
    expert_gain,
    route_ids,
    route_weights,
    expert_gate,
    expert_up,
    expert_down,
):
    length = queries.shape[0]
    experts_count = lax.axis_size(EP)
    place_x = lax.axis_index("x")
    place_y = lax.axis_index("y")
    slot_total = experts_count * CAP
    features = expert_gain.shape[0]
    piece = expert_input.shape[1]
    hid = expert_gate.shape[2]

    cosine_table, sine_table = turn_tables(lax.axis_index(EP) * length, length)
    key_turned = norm_turn(key_rows, key_gain, cosine_table, sine_table)
    key_value = jnp.concatenate([key_turned, values], axis=1)
    key_value = lax.all_gather(key_value, EP, axis=0, tiled=False)
    key_value = key_value.reshape(experts_count * length, 2 * HEAD)
    query_turned = norm_turn(queries, query_gain, cosine_table, sine_table)

    copies = length * 2
    flat_ids = route_ids.reshape(copies)
    hit_marks = (flat_ids[:, None] == jnp.arange(experts_count, dtype=jnp.int32)[None, :]).astype(
        jnp.int32
    )
    earlier = jnp.cumsum(hit_marks, axis=0) - hit_marks
    places = jnp.sum(earlier * hit_marks, axis=1)
    slot_index = (flat_ids * CAP + places).reshape(length, 2)
    slot_axis = jnp.arange(slot_total, dtype=jnp.int32)
    pick = (
        (slot_index[:, 0][None, :] == slot_axis[:, None])
        | (slot_index[:, 1][None, :] == slot_axis[:, None])
    ).astype(BF16)
    outgoing = jnp.dot(pick, expert_input, preferred_element_type=F32).astype(BF16)
    arrived = swap(outgoing.reshape(experts_count, CAP, piece), EP).reshape(slot_total, piece)

    gate_view = expert_gate.reshape(SIDE, SIDE, piece, hid)
    up_view = expert_up.reshape(SIDE, SIDE, piece, hid)

    def first_chunk(k):
        pair = [lax.dynamic_index_in_dim(w, k, 1, keepdims=False) for w in (gate_view, up_view)]
        return jnp.concatenate(pair, axis=2).reshape(SIDE * piece, 2 * hid)

    def second_chunk(k):
        down = lax.dynamic_slice_in_dim(expert_down[0], k * SIDE * hid, SIDE * hid, 0)
        out = lax.dynamic_slice_in_dim(out_weight, k * SIDE * 2 * HEAD, SIDE * 2 * HEAD, 0)
        return jnp.concatenate([down, out], axis=0)

    first_weights = deal(first_chunk, "x")
    second_weights = deal(second_chunk, "y")

    gathered = copies_to(arrived, "y")
    gains = lax.dynamic_index_in_dim(
        expert_gain.reshape(SIDE, SIDE, piece), place_x, axis=1, keepdims=False
    )
    gathered_float = gathered.astype(F32)
    scaled = (gathered_float * gains[:, None, :]).astype(BF16)
    squares = jnp.sum(gathered_float * gathered_float, axis=(0, 2))
    partial = jnp.einsum(
        "ysf,xyfh->xsh",
        scaled,
        first_weights.reshape(SIDE, SIDE, piece, 2 * hid),
        preferred_element_type=F32,
    ).astype(BF16)
    stat_count = -(-slot_total // piece)
    stats = jnp.broadcast_to(stat_rows(squares, stat_count)[None], (SIDE, 2 * stat_count, piece))
    received = swap(jnp.concatenate([partial, stats], axis=1), "x")
    sums = jnp.sum(received[:, :slot_total].astype(F32), axis=0)
    square_sum = read_stat(received[:, slot_total:], stat_count, slot_total)
    row_stat = lax.rsqrt(square_sum / features + EPS)
    gate_value = sums[:, :hid] * row_stat[:, None]
    up_value = sums[:, hid:] * row_stat[:, None]
    hidden = (jax.nn.silu(gate_value) * up_value).astype(BF16)

    hidden_all = copies_to(hidden, "x")
    down_rows = second_weights[:, : SIDE * hid].reshape(SIDE, SIDE, hid, piece)
    out_rows = second_weights[:, SIDE * hid :].reshape(SIDE, SIDE, 2 * HEAD, piece)
    expert_partial = jnp.einsum(
        "xsh,yxhf->ysf", hidden_all, down_rows, preferred_element_type=F32
    ).astype(BF16)
    landed = swap(expert_partial, "y")
    expert_out = jnp.sum(landed.astype(F32), axis=0).astype(BF16)

    heads_out = attend(query_turned, key_value)
    near = jnp.stack([heads_out] + [shift(heads_out, "x", by) for by in range(1, SIDE)])
    heads = in_order(near, place_x)
    head_float = heads.astype(F32)
    mix_gains = lax.dynamic_index_in_dim(
        mix_gain.reshape(SIDE, SIDE, 2 * HEAD), place_y, axis=0, keepdims=False
    )
    mix_in = (head_float * mix_gains[:, None, :]).astype(BF16)
    mix_squares = jnp.sum(head_float * head_float, axis=(0, 2))
    mix_partial = jnp.einsum(
        "xsh,yxhf->ysf", mix_in, out_rows, preferred_element_type=F32
    ).astype(BF16)
    mix_stats = jnp.broadcast_to(stat_rows(mix_squares, 1)[None], (SIDE, 2, piece))
    payload = jnp.concatenate([mix_partial, mix_stats], axis=1)

    def payload_of(k):
        return lax.dynamic_index_in_dim(payload, k, 0, keepdims=False)

    parts = [payload_of(place_y)] + [
        shift(payload_of((place_y + by) % SIDE), "y", by) for by in range(1, SIDE)
    ]
    mix_sum = sum(part[:length].astype(F32) for part in parts)
    mix_square_sum = read_stat(jnp.stack([part[length:] for part in parts]), 1, length)
    mix_scale = lax.rsqrt(mix_square_sum / mix_gain.shape[0] + EPS)
    attended = (mix_sum * mix_scale[:, None]).astype(BF16)

    returned = swap(expert_out.reshape(experts_count, CAP, piece), EP).reshape(slot_total, piece)
    slots = slot_axis[None, :]
    first = jnp.dot(
        (slot_index[:, :1] == slots).astype(BF16), returned, preferred_element_type=F32
    )
    second = jnp.dot(
        (slot_index[:, 1:] == slots).astype(BF16), returned, preferred_element_type=F32
    )
    expert_mix = (first * route_weights[:, :1] + second * route_weights[:, 1:]).astype(BF16)
    return (attended, expert_mix)


def solution(mesh):
    torus = Mesh(mesh.devices.reshape(-1, 2, SIDE, SIDE), ("z", "c", "y", "x"))
    return jax.shard_map(
        forward,
        mesh=torus,
        in_specs=(
            P(EP, TP),
            P(EP, TP),
            P(EP, TP),
            P(),
            P(),
            P(),
            P(None, TP),
            P(EP, TP),
            P(),
            P(EP, None),
            P(EP, None),
            P(EP, None, TP),
            P(EP, None, TP),
            P(EP, None, TP),
        ),
        out_specs=(P(EP, TP), P(EP, TP)),
        check_vma=False,
    )
```

```python
import functools

import jax
import jax.numpy as jnp
from jax import lax
from jax.experimental import pallas as pl
from jax.experimental.pallas import tpu as pltpu
from jax.sharding import Mesh
from jax.sharding import PartitionSpec as P


HEAD = 64
GRID_W = 64
EPS = 1e-06
THETA = 10000.0
EP = ("z", "c")
TP = ("y", "x")
SIDE = 4
CAP = 22
STAT_ROWS = 16
KEY_STEP = 2048

F32 = jnp.float32
BF16 = jnp.bfloat16


def turn_tables(offset, length):
    half_width = HEAD // 2
    inverse = THETA ** (-jnp.arange(0, half_width, 2, dtype=F32) / half_width)
    positions = offset + jnp.arange(length, dtype=jnp.int32)
    lane = jnp.arange(2 * HEAD, dtype=jnp.int32) % HEAD
    grid_rows = (positions // GRID_W).astype(F32)[:, None]
    grid_cols = (positions % GRID_W).astype(F32)[:, None]
    step = jnp.tile(jnp.repeat(jnp.concatenate([inverse, inverse]), 2), 2)
    angles = jnp.where(lane < half_width, grid_rows, grid_cols) * step
    sign = jnp.where(lane % 2 == 0, -1.0, 1.0)
    return jnp.cos(angles), jnp.sin(angles) * sign


def turn_body(q_ref, kv_ref, q_gain_ref, k_gain_ref, cos_ref, sin_ref, q_out, kv_out):
    shape = q_ref.shape
    lane = lax.broadcasted_iota(jnp.int32, shape, 1)
    low = lane < HEAD
    even = lane % 2 == 0

    def turned(rows, gain):
        squares = rows * rows
        first = jnp.sum(jnp.where(low, squares, 0.0), axis=1, keepdims=True) / HEAD
        second = jnp.sum(jnp.where(low, 0.0, squares), axis=1, keepdims=True) / HEAD
        gain = jnp.concatenate([gain, gain], axis=1)
        rows = rows * jnp.where(low, lax.rsqrt(first + EPS), lax.rsqrt(second + EPS)) * gain
        swapped = jnp.where(even, pltpu.roll(rows, 2 * HEAD - 1, 1), pltpu.roll(rows, 1, 1))
        return (rows * cos_ref[...] + swapped * sin_ref[...]).astype(BF16)

    q_out[...] = turned(q_ref[...].astype(F32), q_gain_ref[...])
    both = kv_ref[...]
    kv_out[...] = jnp.where(low, turned(both.astype(F32), k_gain_ref[...]), both)


def turn(queries, key_value, query_gain, key_gain, tables):
    shape = jax.ShapeDtypeStruct(queries.shape, BF16)
    return pl.pallas_call(turn_body, out_shape=[shape, shape], name="turn")(
        queries,
        key_value,
        query_gain[None, :],
        key_gain[None, :],
        *tables,
    )


def attend_body(q_ref, kv_ref, out_ref):
    rows = q_ref.shape[0]
    lanes = lax.broadcasted_iota(jnp.int32, (rows, 2 * HEAD), 1)
    both = q_ref[...].astype(F32)
    low = jnp.where(lanes < HEAD, both, 0.0)
    high = pltpu.roll(jnp.where(lanes < HEAD, 0.0, both), HEAD, 1)
    wide = (jnp.concatenate([low, high], axis=0) * 0.125).astype(BF16)
    top = jnp.full((2 * rows, 1), -jnp.inf, F32)
    total = jnp.zeros((2 * rows, 1), F32)
    acc = jnp.zeros((2 * rows, 2 * HEAD), F32)
    for at in range(0, kv_ref.shape[0], KEY_STEP):
        block = kv_ref[at : at + KEY_STEP, :]
        scores = lax.dot_general(wide, block, (((1,), (1,)), ((), ())), preferred_element_type=F32)
        new_top = jnp.maximum(top, jnp.max(scores, axis=1, keepdims=True))
        factor = jnp.exp(top - new_top)
        raw = jnp.exp(scores - new_top)
        total = total * factor + jnp.sum(raw, axis=1, keepdims=True)
        acc = acc * factor + jnp.dot(raw.astype(BF16), block, preferred_element_type=F32)
        top = new_top
    done = acc / total
    first = pltpu.roll(done[:rows], HEAD, 1)
    out_ref[...] = jnp.where(lanes < HEAD, first, done[rows:]).astype(BF16)


def attend(query_turned, key_value):
    rows = query_turned.shape[0]
    keys = key_value.shape[0]
    return pl.pallas_call(
        attend_body,
        out_shape=jax.ShapeDtypeStruct(query_turned.shape, BF16),
        compiler_params=pltpu.CompilerParams(vmem_limit_bytes=48 * 1024 * 1024),
        cost_estimate=pl.CostEstimate(
            flops=16 * rows * keys * HEAD,
            bytes_accessed=keys * 4 * HEAD,
            transcendentals=2 * rows * keys,
        ),
        name="attend",
    )(query_turned, key_value)


def mix_body(k_rows, base, joined, index_ref, *refs):
    if joined:
        pieces, refs = [refs[0].at[q] for q in range(SIDE)], refs[1:]
        outs = [refs[-1].at[index_ref[2 * SIDE + r]] for r in range(SIDE)]
    else:
        pieces, outs, refs = refs[:SIDE], refs[-SIDE:], refs[SIDE:]
    weights, gain_ref = refs[:SIDE], refs[SIDE]
    rows = pieces[0].shape[0]
    scaled = [
        (pieces[q][...].astype(F32) * gain_ref[pl.ds(index_ref[SIDE + q], 1), :]).astype(BF16)
        for q in range(SIDE)
    ]
    for r in range(SIDE):
        total = jnp.zeros((rows, weights[r].shape[1]), F32)
        for q in range(SIDE):
            block = weights[r][pl.ds(pl.multiple_of(base + index_ref[q] * k_rows, 128), k_rows), :]
            total += jnp.dot(scaled[q], block, preferred_element_type=F32)
        outs[r][:rows, :] = total.astype(BF16)
    squares = jnp.zeros((rows, k_rows), F32)
    for q in range(SIDE):
        values = pieces[q][...].astype(F32)
        squares += values * values
    high = squares.astype(BF16)
    low = (squares - high.astype(F32)).astype(BF16)
    ones = jnp.ones((8, k_rows), BF16)
    sums = jnp.zeros((8, rows), F32)
    for part in (high, low):
        sums += lax.dot_general(ones, part, (((1,), (1,)), ((), ())), preferred_element_type=F32)
    width = outs[0].shape[1]
    count = -(-rows // width)
    if count * width > rows:
        sums = jnp.concatenate([sums, jnp.zeros((8, count * width - rows), F32)], axis=1)
    line = lax.broadcasted_iota(jnp.int32, (STAT_ROWS, width), 0)
    block = jnp.zeros((STAT_ROWS, width), F32)
    for j in range(count):
        value = sums[0:1, j * width : (j + 1) * width]
        high = value.astype(BF16).astype(F32)
        block = jnp.where(line == j, high, block)
        block = jnp.where(line == count + j, value - high, block)
    for r in range(SIDE):
        outs[r][rows:, :] = block.astype(BF16)


def mix(pieces, weights, base, gains, indices):
    joined = not isinstance(pieces, list)
    rows, k_rows = pieces[0].shape
    width = weights[0].shape[1]
    vmem = pl.BlockSpec(memory_space=pltpu.VMEM)
    shape = (rows + STAT_ROWS, width)
    given = [pieces] if joined else pieces
    return pl.pallas_call(
        functools.partial(mix_body, k_rows, base, joined),
        out_shape=jax.ShapeDtypeStruct((SIDE,) + shape, BF16)
        if joined
        else [jax.ShapeDtypeStruct(shape, BF16)] * SIDE,
        in_specs=[pl.BlockSpec(memory_space=pltpu.SMEM)] + [vmem] * (len(given) + SIDE + 1),
        out_specs=vmem if joined else [vmem] * SIDE,
        compiler_params=pltpu.CompilerParams(vmem_limit_bytes=48 * 1024 * 1024),
        cost_estimate=pl.CostEstimate(
            flops=2 * SIDE * SIDE * rows * k_rows * width,
            bytes_accessed=SIDE * rows * (k_rows + width) * 2,
            transcendentals=0,
        ),
    )(jnp.concatenate(indices), *given, *weights, gains)


def hidden_body(features, in_ref, out_ref):
    rows = out_ref.shape[1]
    hid = out_ref.shape[2]
    width = 2 * hid
    count = -(-rows // width)
    stats = sum(in_ref[k, rows:, :].astype(F32) for k in range(SIDE))
    for j in range(count):
        first, last = j * width, min(rows, (j + 1) * width)
        line = stats[j : j + 1, :] + stats[count + j : count + j + 1, :]
        scale = lax.rsqrt(line / features + EPS)
        column = jnp.transpose(jnp.broadcast_to(scale, (8, width)))[: last - first, 0:1]
        sums = sum(in_ref[k, first:last, :].astype(F32) for k in range(SIDE))
        gate = sums[:, :hid] * column
        up = sums[:, hid:] * column
        result = (gate / (1.0 + jnp.exp(-gate)) * up).astype(BF16)
        for k in range(SIDE):
            out_ref[k, first:last, :] = result


def second_body(index_ref, gathered, *refs):
    weights, out_ref = refs[:SIDE], refs[-1]
    hid = gathered.shape[2]
    wide = jnp.concatenate([gathered[k] for k in range(SIDE)], axis=1)
    for r in range(SIDE):
        out_ref[index_ref[r]] = jnp.dot(
            wide, weights[r][: SIDE * hid, :], preferred_element_type=F32
        ).astype(BF16)


def read_stat(rows, count, size):
    whole = rows.astype(F32)
    return jnp.sum(whole[:, :count] + whole[:, count : 2 * count], axis=0).reshape(-1)[:size]


def send_back(parts, axis):
    return [parts[0]] + [shift(parts[r], axis, SIDE - r) for r in range(1, SIDE)]


def copies_to(array, axis):
    wide = jnp.broadcast_to(array[None], (SIDE,) + array.shape)
    return swap(wide, axis)


def swap(array, axis):
    return lax.all_to_all(array, axis, 0, 0, tiled=True)


def shift(array, axis, by):
    size = lax.axis_size(axis)
    return lax.ppermute(array, axis, [(k, (k + by) % size) for k in range(size)])


def deal(chunk_for, axis):
    place = lax.axis_index(axis)
    landed = [chunk_for(place)]
    for by in range(1, SIDE):
        landed.append(shift(chunk_for((place + by) % SIDE), axis, by))
    return landed


def forward(
    queries,
    key_rows,
    values,
    query_gain,
    key_gain,
    mix_gain,
    out_weight,
    expert_input,
    expert_gain,
    route_ids,
    route_weights,
    expert_gate,
    expert_up,
    expert_down,
):
    length = queries.shape[0]
    experts_count = lax.axis_size(EP)
    place_x = lax.axis_index("x")
    place_y = lax.axis_index("y")
    slot_total = experts_count * CAP
    features = expert_gain.shape[0]
    piece = expert_input.shape[1]
    hid = expert_gate.shape[2]

    tables = turn_tables(lax.axis_index(EP) * length, length)
    query_turned, own_rows = turn(
        queries, jnp.concatenate([key_rows, values], axis=1), query_gain, key_gain, tables
    )
    key_value = lax.all_gather(own_rows, EP, axis=0, tiled=False)
    key_value = key_value.reshape(experts_count * length, 2 * HEAD)

    copies = length * 2
    flat_ids = route_ids.reshape(copies)
    hit_marks = (flat_ids[:, None] == jnp.arange(experts_count, dtype=jnp.int32)[None, :]).astype(
        jnp.int32
    )
    earlier = jnp.cumsum(hit_marks, axis=0) - hit_marks
    places = jnp.sum(earlier * hit_marks, axis=1)
    slot_index = (flat_ids * CAP + places).reshape(length, 2)
    slot_axis = jnp.arange(slot_total, dtype=jnp.int32)
    pick = (
        (slot_index[:, 0][None, :] == slot_axis[:, None])
        | (slot_index[:, 1][None, :] == slot_axis[:, None])
    ).astype(BF16)
    outgoing = jnp.dot(pick, expert_input, preferred_element_type=F32).astype(BF16)
    arrived = swap(outgoing.reshape(experts_count, CAP, piece), EP).reshape(slot_total, piece)

    gate_view = expert_gate.reshape(SIDE, SIDE, piece, hid)
    up_view = expert_up.reshape(SIDE, SIDE, piece, hid)

    def first_chunk(k):
        pair = [lax.dynamic_index_in_dim(w, k, 1, keepdims=False) for w in (gate_view, up_view)]
        return jnp.concatenate(pair, axis=2).reshape(SIDE * piece, 2 * hid)

    def second_chunk(k):
        down = lax.dynamic_slice_in_dim(expert_down[0], k * SIDE * hid, SIDE * hid, 0)
        out = lax.dynamic_slice_in_dim(out_weight, k * SIDE * 2 * HEAD, SIDE * 2 * HEAD, 0)
        return jnp.concatenate([down, out], axis=0)

    first_weights = deal(first_chunk, "x")
    second_weights = deal(second_chunk, "y")

    ahead = jnp.arange(SIDE, dtype=jnp.int32)
    from_y = (place_y - ahead) % SIDE
    from_x = (place_x - ahead) % SIDE
    partial = mix(
        copies_to(arrived, "y"),
        first_weights,
        0,
        expert_gain.reshape(SIDE * SIDE, piece),
        (ahead, ahead * SIDE + place_x, from_x),
    )
    sums = swap(partial, "x")
    hidden = pl.pallas_call(
        functools.partial(hidden_body, features),
        out_shape=jax.ShapeDtypeStruct((SIDE, slot_total, hid), BF16),
        compiler_params=pltpu.CompilerParams(vmem_limit_bytes=48 * 1024 * 1024),
        name="hidden",
    )(sums)

    hidden_all = swap(hidden, "x")
    vmem = pl.BlockSpec(memory_space=pltpu.VMEM)
    expert_partial = pl.pallas_call(
        second_body,
        out_shape=jax.ShapeDtypeStruct((SIDE, slot_total, piece), BF16),
        in_specs=[pl.BlockSpec(memory_space=pltpu.SMEM)] + [vmem] * (1 + SIDE),
        out_specs=vmem,
        compiler_params=pltpu.CompilerParams(vmem_limit_bytes=48 * 1024 * 1024),
        name="second",
    )(from_y, hidden_all, *second_weights)
    landed = swap(expert_partial, "y")
    expert_out = jnp.sum(landed.astype(F32), axis=0).astype(BF16)

    heads_out = attend(query_turned, key_value)
    heads = [heads_out] + [shift(heads_out, "x", by) for by in range(1, SIDE)]
    mix_partial = mix(
        heads,
        second_weights,
        SIDE * hid,
        mix_gain.reshape(SIDE * SIDE, 2 * HEAD),
        (from_x, place_y * SIDE + from_x),
    )
    parts = send_back(mix_partial, "y")
    mix_sum = sum(part[:length].astype(F32) for part in parts)
    mix_square_sum = read_stat(jnp.stack([part[length:] for part in parts]), 1, length)
    mix_scale = lax.rsqrt(mix_square_sum / mix_gain.shape[0] + EPS)
    attended = (mix_sum * mix_scale[:, None]).astype(BF16)

    returned = swap(expert_out.reshape(experts_count, CAP, piece), EP).reshape(slot_total, piece)
    slots = slot_axis[None, :]
    first = jnp.dot(
        (slot_index[:, :1] == slots).astype(BF16), returned, preferred_element_type=F32
    )
    second = jnp.dot(
        (slot_index[:, 1:] == slots).astype(BF16), returned, preferred_element_type=F32
    )
    expert_mix = (first * route_weights[:, :1] + second * route_weights[:, 1:]).astype(BF16)
    return (attended, expert_mix)


def solution(mesh):
    torus = Mesh(mesh.devices.reshape(-1, 2, SIDE, SIDE), ("z", "c", "y", "x"))
    return jax.shard_map(
        forward,
        mesh=torus,
        in_specs=(
            P(EP, TP),
            P(EP, TP),
            P(EP, TP),
            P(),
            P(),
            P(),
            P(None, TP),
            P(EP, TP),
            P(),
            P(EP, None),
            P(EP, None),
            P(EP, None, TP),
            P(EP, None, TP),
            P(EP, None, TP),
        ),
        out_specs=(P(EP, TP), P(EP, TP)),
        check_vma=False,
    )
```

```python
import functools

import jax
import jax.numpy as jnp
from jax import lax
from jax.experimental import pallas as pl
from jax.experimental.pallas import tpu as pltpu
from jax.sharding import Mesh
from jax.sharding import PartitionSpec as P


HEAD = 64
GRID_W = 64
EPS = 1e-06
THETA = 10000.0
EP = ("z", "c")
TP = ("y", "x")
SIDE = 4
CAP = 22
STAT_ROWS = 16
KEY_STEP = 2048

F32 = jnp.float32
BF16 = jnp.bfloat16


def turn_tables(offset, length):
    half_width = HEAD // 2
    inverse = THETA ** (-jnp.arange(0, half_width, 2, dtype=F32) / half_width)
    positions = offset + jnp.arange(length, dtype=jnp.int32)
    lane = jnp.arange(2 * HEAD, dtype=jnp.int32) % HEAD
    grid_rows = (positions // GRID_W).astype(F32)[:, None]
    grid_cols = (positions % GRID_W).astype(F32)[:, None]
    step = jnp.tile(jnp.repeat(jnp.concatenate([inverse, inverse]), 2), 2)
    angles = jnp.where(lane < half_width, grid_rows, grid_cols) * step
    sign = jnp.where(lane % 2 == 0, -1.0, 1.0)
    return jnp.cos(angles), jnp.sin(angles) * sign


def turn_body(q_ref, kv_ref, q_gain_ref, k_gain_ref, cos_ref, sin_ref, q_out, kv_out):
    shape = q_ref.shape
    lane = lax.broadcasted_iota(jnp.int32, shape, 1)
    low = lane < HEAD
    even = lane % 2 == 0

    def turned(rows, gain):
        squares = rows * rows
        first = jnp.sum(jnp.where(low, squares, 0.0), axis=1, keepdims=True) / HEAD
        second = jnp.sum(jnp.where(low, 0.0, squares), axis=1, keepdims=True) / HEAD
        gain = jnp.concatenate([gain, gain], axis=1)
        rows = rows * jnp.where(low, lax.rsqrt(first + EPS), lax.rsqrt(second + EPS)) * gain
        swapped = jnp.where(even, pltpu.roll(rows, 2 * HEAD - 1, 1), pltpu.roll(rows, 1, 1))
        return (rows * cos_ref[...] + swapped * sin_ref[...]).astype(BF16)

    q_out[...] = turned(q_ref[...].astype(F32), q_gain_ref[...])
    both = kv_ref[...]
    kv_out[...] = jnp.where(low, turned(both.astype(F32), k_gain_ref[...]), both)


def turn(queries, key_value, query_gain, key_gain, tables):
    shape = jax.ShapeDtypeStruct(queries.shape, BF16)
    return pl.pallas_call(turn_body, out_shape=[shape, shape], name="turn")(
        queries,
        key_value,
        query_gain[None, :],
        key_gain[None, :],
        *tables,
    )


def attend_body(q_ref, mine_ref, other_ref, out_ref):
    rows = q_ref.shape[0]
    lanes = lax.broadcasted_iota(jnp.int32, (rows, 2 * HEAD), 1)
    both = q_ref[...].astype(F32)
    low = jnp.where(lanes < HEAD, both, 0.0)
    high = pltpu.roll(jnp.where(lanes < HEAD, 0.0, both), HEAD, 1)
    wide = (jnp.concatenate([low, high], axis=0) * 0.125).astype(BF16)
    top = jnp.full((2 * rows, 1), -jnp.inf, F32)
    total = jnp.zeros((2 * rows, 1), F32)
    acc = jnp.zeros((2 * rows, 2 * HEAD), F32)
    steps = [
        (ref, at) for ref in (mine_ref, other_ref) for at in range(0, ref.shape[0], KEY_STEP)
    ]
    for ref, at in steps:
        block = ref[at : at + KEY_STEP, :]
        scores = lax.dot_general(wide, block, (((1,), (1,)), ((), ())), preferred_element_type=F32)
        new_top = jnp.maximum(top, jnp.max(scores, axis=1, keepdims=True))
        factor = jnp.exp(top - new_top)
        raw = jnp.exp(scores - new_top)
        total = total * factor + jnp.sum(raw, axis=1, keepdims=True)
        acc = acc * factor + jnp.dot(raw.astype(BF16), block, preferred_element_type=F32)
        top = new_top
    done = acc / total
    first = pltpu.roll(done[:rows], HEAD, 1)
    out_ref[...] = jnp.where(lanes < HEAD, first, done[rows:]).astype(BF16)


def attend(query_turned, mine, other):
    rows = query_turned.shape[0]
    keys = mine.shape[0] + other.shape[0]
    return pl.pallas_call(
        attend_body,
        out_shape=jax.ShapeDtypeStruct(query_turned.shape, BF16),
        compiler_params=pltpu.CompilerParams(vmem_limit_bytes=48 * 1024 * 1024),
        cost_estimate=pl.CostEstimate(
            flops=16 * rows * keys * HEAD,
            bytes_accessed=keys * 4 * HEAD,
            transcendentals=2 * rows * keys,
        ),
        name="attend",
    )(query_turned, mine, other)


def route_body(ids_ref, rows_ref, out_ref, slot_ref):
    blocks, cap, _ = out_ref.shape
    count = rows_ref.shape[0]
    lane = lax.broadcasted_iota(jnp.int32, (count, blocks), 1)
    ids = [ids_ref[:, k : k + 1] for k in range(2)]
    marks = [(lane == ids[k]).astype(F32) for k in range(2)]
    down = lax.broadcasted_iota(jnp.int32, (count, count), 0)
    across = lax.broadcasted_iota(jnp.int32, (count, count), 1)
    below = (across < down).astype(BF16)
    earlier = jnp.dot(below, (marks[0] + marks[1]).astype(BF16), preferred_element_type=F32)
    places = [
        jnp.sum(earlier * marks[0], axis=1, keepdims=True),
        jnp.sum((earlier + marks[0]) * marks[1], axis=1, keepdims=True),
    ]
    slots = [ids[k] * cap + places[k].astype(jnp.int32) for k in range(2)]
    slot_ref[...] = jnp.concatenate(slots, axis=1)
    slot = lax.broadcasted_iota(jnp.int32, (count, blocks * cap), 1)
    pick = ((slot == slots[0]) | (slot == slots[1])).astype(BF16)
    placed = lax.dot_general(
        pick, rows_ref[...], (((0,), (0,)), ((), ())), preferred_element_type=F32
    )
    for k in range(blocks):
        out_ref[k] = placed[k * cap : (k + 1) * cap, :].astype(BF16)


def mix_body(k_rows, base, joined, index_ref, *refs):
    if joined:
        pieces, refs = [refs[0].at[q] for q in range(SIDE)], refs[1:]
        outs = [refs[-1].at[index_ref[2 * SIDE + r]] for r in range(SIDE)]
    else:
        pieces, outs, refs = refs[:SIDE], refs[-SIDE:], refs[SIDE:]
    weights, gain_ref = refs[:SIDE], refs[SIDE]
    rows = pieces[0].shape[0]
    scaled = [
        (pieces[q][...].astype(F32) * gain_ref[pl.ds(index_ref[SIDE + q], 1), :]).astype(BF16)
        for q in range(SIDE)
    ]
    for r in range(SIDE):
        total = jnp.zeros((rows, weights[r].shape[1]), F32)
        for q in range(SIDE):
            block = weights[r][pl.ds(pl.multiple_of(base + index_ref[q] * k_rows, 128), k_rows), :]
            total += jnp.dot(scaled[q], block, preferred_element_type=F32)
        outs[r][:rows, :] = total.astype(BF16)
    squares = jnp.zeros((rows, k_rows), F32)
    for q in range(SIDE):
        values = pieces[q][...].astype(F32)
        squares += values * values
    high = squares.astype(BF16)
    low = (squares - high.astype(F32)).astype(BF16)
    ones = jnp.ones((8, k_rows), BF16)
    sums = jnp.zeros((8, rows), F32)
    for part in (high, low):
        sums += lax.dot_general(ones, part, (((1,), (1,)), ((), ())), preferred_element_type=F32)
    width = outs[0].shape[1]
    count = -(-rows // width)
    if count * width > rows:
        sums = jnp.concatenate([sums, jnp.zeros((8, count * width - rows), F32)], axis=1)
    line = lax.broadcasted_iota(jnp.int32, (STAT_ROWS, width), 0)
    block = jnp.zeros((STAT_ROWS, width), F32)
    for j in range(count):
        value = sums[0:1, j * width : (j + 1) * width]
        high = value.astype(BF16).astype(F32)
        block = jnp.where(line == j, high, block)
        block = jnp.where(line == count + j, value - high, block)
    for r in range(SIDE):
        outs[r][rows:, :] = block.astype(BF16)


def mix(pieces, weights, base, gains, indices):
    joined = not isinstance(pieces, list)
    rows, k_rows = pieces[0].shape
    width = weights[0].shape[1]
    vmem = pl.BlockSpec(memory_space=pltpu.VMEM)
    shape = (rows + STAT_ROWS, width)
    given = [pieces] if joined else pieces
    return pl.pallas_call(
        functools.partial(mix_body, k_rows, base, joined),
        out_shape=jax.ShapeDtypeStruct((SIDE,) + shape, BF16)
        if joined
        else [jax.ShapeDtypeStruct(shape, BF16)] * SIDE,
        in_specs=[pl.BlockSpec(memory_space=pltpu.SMEM)] + [vmem] * (len(given) + SIDE + 1),
        out_specs=vmem if joined else [vmem] * SIDE,
        compiler_params=pltpu.CompilerParams(vmem_limit_bytes=48 * 1024 * 1024),
        cost_estimate=pl.CostEstimate(
            flops=2 * SIDE * SIDE * rows * k_rows * width,
            bytes_accessed=SIDE * rows * (k_rows + width) * 2,
            transcendentals=0,
        ),
    )(jnp.concatenate(indices), *given, *weights, gains)


def hidden_body(features, in_ref, out_ref):
    rows = out_ref.shape[1]
    hid = out_ref.shape[2]
    width = 2 * hid
    count = -(-rows // width)
    stats = sum(in_ref[k, rows:, :].astype(F32) for k in range(SIDE))
    for j in range(count):
        first, last = j * width, min(rows, (j + 1) * width)
        line = stats[j : j + 1, :] + stats[count + j : count + j + 1, :]
        scale = lax.rsqrt(line / features + EPS)
        column = jnp.transpose(jnp.broadcast_to(scale, (8, width)))[: last - first, 0:1]
        sums = sum(in_ref[k, first:last, :].astype(F32) for k in range(SIDE))
        gate = sums[:, :hid] * column
        up = sums[:, hid:] * column
        result = (gate / (1.0 + jnp.exp(-gate)) * up).astype(BF16)
        for k in range(SIDE):
            out_ref[k, first:last, :] = result


def second_body(index_ref, gathered, *refs):
    weights, out_ref = refs[:SIDE], refs[-1]
    hid = gathered.shape[2]
    wide = jnp.concatenate([gathered[k] for k in range(SIDE)], axis=1)
    for r in range(SIDE):
        out_ref[index_ref[r]] = jnp.dot(
            wide, weights[r][: SIDE * hid, :], preferred_element_type=F32
        ).astype(BF16)


def read_stat(rows, count, size):
    whole = rows.astype(F32)
    return jnp.sum(whole[:, :count] + whole[:, count : 2 * count], axis=0).reshape(-1)[:size]


def send_back(parts, axis):
    return [parts[0]] + [shift(parts[r], axis, SIDE - r) for r in range(1, SIDE)]


def copies_to(array, axis):
    wide = jnp.broadcast_to(array[None], (SIDE,) + array.shape)
    return swap(wide, axis)


def swap(array, axis):
    return lax.all_to_all(array, axis, 0, 0, tiled=True)


def shift(array, axis, by):
    size = lax.axis_size(axis)
    return lax.ppermute(array, axis, [(k, (k + by) % size) for k in range(size)])


def keys_everywhere(mine):
    by = lax.axis_size("z") // 2
    while by:
        came = shift(mine, "z", by)
        mine = jnp.concatenate([mine, came], axis=0)
        by //= 2
    return mine, shift(mine, "c", 1)


def deal(chunk_for, axis):
    place = lax.axis_index(axis)
    landed = [chunk_for(place)]
    for by in range(1, SIDE):
        landed.append(shift(chunk_for((place + by) % SIDE), axis, by))
    return landed


def forward(
    queries,
    key_rows,
    values,
    query_gain,
    key_gain,
    mix_gain,
    out_weight,
    expert_input,
    expert_gain,
    route_ids,
    route_weights,
    expert_gate,
    expert_up,
    expert_down,
):
    length = queries.shape[0]
    experts_count = lax.axis_size(EP)
    place_x = lax.axis_index("x")
    place_y = lax.axis_index("y")
    slot_total = experts_count * CAP
    features = expert_gain.shape[0]
    piece = expert_input.shape[1]
    hid = expert_gate.shape[2]

    tables = turn_tables(lax.axis_index(EP) * length, length)
    query_turned, own_rows = turn(
        queries, jnp.concatenate([key_rows, values], axis=1), query_gain, key_gain, tables
    )
    mine, other = keys_everywhere(own_rows)

    outgoing, slot_index = pl.pallas_call(
        route_body,
        out_shape=[
            jax.ShapeDtypeStruct((experts_count, CAP, piece), BF16),
            jax.ShapeDtypeStruct((length, 2), jnp.int32),
        ],
        name="route",
    )(route_ids, expert_input)
    arrived = swap(outgoing, EP).reshape(slot_total, piece)

    gate_view = expert_gate.reshape(SIDE, SIDE, piece, hid)
    up_view = expert_up.reshape(SIDE, SIDE, piece, hid)

    def first_chunk(k):
        pair = [lax.dynamic_index_in_dim(w, k, 1, keepdims=False) for w in (gate_view, up_view)]
        return jnp.concatenate(pair, axis=2).reshape(SIDE * piece, 2 * hid)

    def second_chunk(k):
        down = lax.dynamic_slice_in_dim(expert_down[0], k * SIDE * hid, SIDE * hid, 0)
        out = lax.dynamic_slice_in_dim(out_weight, k * SIDE * 2 * HEAD, SIDE * 2 * HEAD, 0)
        return jnp.concatenate([down, out], axis=0)

    first_weights = deal(first_chunk, "x")
    second_weights = deal(second_chunk, "y")

    ahead = jnp.arange(SIDE, dtype=jnp.int32)
    from_y = (place_y - ahead) % SIDE
    from_x = (place_x - ahead) % SIDE
    partial = mix(
        copies_to(arrived, "y"),
        first_weights,
        0,
        expert_gain.reshape(SIDE * SIDE, piece),
        (ahead, ahead * SIDE + place_x, from_x),
    )
    sums = swap(partial, "x")
    hidden = pl.pallas_call(
        functools.partial(hidden_body, features),
        out_shape=jax.ShapeDtypeStruct((SIDE, slot_total, hid), BF16),
        compiler_params=pltpu.CompilerParams(vmem_limit_bytes=48 * 1024 * 1024),
        name="hidden",
    )(sums)

    hidden_all = swap(hidden, "x")
    vmem = pl.BlockSpec(memory_space=pltpu.VMEM)
    expert_partial = pl.pallas_call(
        second_body,
        out_shape=jax.ShapeDtypeStruct((SIDE, slot_total, piece), BF16),
        in_specs=[pl.BlockSpec(memory_space=pltpu.SMEM)] + [vmem] * (1 + SIDE),
        out_specs=vmem,
        compiler_params=pltpu.CompilerParams(vmem_limit_bytes=48 * 1024 * 1024),
        name="second",
    )(from_y, hidden_all, *second_weights)
    landed = swap(expert_partial, "y")
    expert_out = jnp.sum(landed.astype(F32), axis=0).astype(BF16)
    expert_out = expert_out.reshape(experts_count, CAP, piece)

    heads_out = attend(query_turned, mine, other)
    heads = [heads_out] + [shift(heads_out, "x", by) for by in range(1, SIDE)]
    mix_partial = mix(
        heads,
        second_weights,
        SIDE * hid,
        mix_gain.reshape(SIDE * SIDE, 2 * HEAD),
        (from_x, place_y * SIDE + from_x),
    )
    parts = send_back(mix_partial, "y")
    mix_sum = sum(part[:length].astype(F32) for part in parts)
    mix_square_sum = read_stat(jnp.stack([part[length:] for part in parts]), 1, length)
    mix_scale = lax.rsqrt(mix_square_sum / mix_gain.shape[0] + EPS)
    attended = (mix_sum * mix_scale[:, None]).astype(BF16)

    returned = swap(expert_out, EP).reshape(slot_total, piece)
    slots = jnp.arange(slot_total, dtype=jnp.int32)[None, :]
    first = jnp.dot(
        (slot_index[:, :1] == slots).astype(BF16), returned, preferred_element_type=F32
    )
    second = jnp.dot(
        (slot_index[:, 1:] == slots).astype(BF16), returned, preferred_element_type=F32
    )
    expert_mix = (first * route_weights[:, :1] + second * route_weights[:, 1:]).astype(BF16)
    return (attended, expert_mix)


def solution(mesh):
    torus = Mesh(mesh.devices.reshape(-1, 2, SIDE, SIDE), ("z", "c", "y", "x"))
    return jax.shard_map(
        forward,
        mesh=torus,
        in_specs=(
            P(EP, TP),
            P(EP, TP),
            P(EP, TP),
            P(),
            P(),
            P(),
            P(None, TP),
            P(EP, TP),
            P(),
            P(EP, None),
            P(EP, None),
            P(EP, None, TP),
            P(EP, None, TP),
            P(EP, None, TP),
        ),
        out_specs=(P(EP, TP), P(EP, TP)),
        check_vma=False,
    )
```

```python
import functools

import jax
import jax.numpy as jnp
from jax import lax
from jax.experimental import pallas as pl
from jax.experimental.pallas import tpu as pltpu
from jax.sharding import Mesh
from jax.sharding import PartitionSpec as P


HEAD = 64
GRID_W = 64
EPS = 1e-06
THETA = 10000.0
EP = ("z", "c")
TP = ("y", "x")
SIDE = 4
CAP = 22
STAT_ROWS = 16
KEY_STEP = 2048

F32 = jnp.float32
BF16 = jnp.bfloat16


def turn_tables(offset, length):
    half_width = HEAD // 2
    inverse = THETA ** (-jnp.arange(0, half_width, 2, dtype=F32) / half_width)
    positions = offset + jnp.arange(length, dtype=jnp.int32)
    lane = jnp.arange(2 * HEAD, dtype=jnp.int32) % HEAD
    grid_rows = (positions // GRID_W).astype(F32)[:, None]
    grid_cols = (positions % GRID_W).astype(F32)[:, None]
    step = jnp.tile(jnp.repeat(jnp.concatenate([inverse, inverse]), 2), 2)
    angles = jnp.where(lane < half_width, grid_rows, grid_cols) * step
    sign = jnp.where(lane % 2 == 0, -1.0, 1.0)
    return jnp.cos(angles), jnp.sin(angles) * sign


def turn_body(q_ref, kv_ref, q_gain_ref, k_gain_ref, cos_ref, sin_ref, q_out, kv_out):
    shape = q_ref.shape
    lane = lax.broadcasted_iota(jnp.int32, shape, 1)
    low = lane < HEAD
    even = lane % 2 == 0

    def turned(rows, gain):
        squares = rows * rows
        first = jnp.sum(jnp.where(low, squares, 0.0), axis=1, keepdims=True) / HEAD
        second = jnp.sum(jnp.where(low, 0.0, squares), axis=1, keepdims=True) / HEAD
        gain = jnp.concatenate([gain, gain], axis=1)
        rows = rows * jnp.where(low, lax.rsqrt(first + EPS), lax.rsqrt(second + EPS)) * gain
        swapped = jnp.where(even, pltpu.roll(rows, 2 * HEAD - 1, 1), pltpu.roll(rows, 1, 1))
        return (rows * cos_ref[...] + swapped * sin_ref[...]).astype(BF16)

    q_out[...] = turned(q_ref[...].astype(F32), q_gain_ref[...])
    both = kv_ref[...]
    kv_out[...] = jnp.where(low, turned(both.astype(F32), k_gain_ref[...]), both)


def turn(queries, key_value, query_gain, key_gain, tables):
    shape = jax.ShapeDtypeStruct(queries.shape, BF16)
    return pl.pallas_call(turn_body, out_shape=[shape, shape], name="turn")(
        queries,
        key_value,
        query_gain[None, :],
        key_gain[None, :],
        *tables,
    )


def attend_body(q_ref, mine_ref, other_ref, out_ref):
    rows = q_ref.shape[0]
    lanes = lax.broadcasted_iota(jnp.int32, (rows, 2 * HEAD), 1)
    both = q_ref[...].astype(F32)
    low = jnp.where(lanes < HEAD, both, 0.0)
    high = pltpu.roll(jnp.where(lanes < HEAD, 0.0, both), HEAD, 1)
    wide = (jnp.concatenate([low, high], axis=0) * 0.125).astype(BF16)
    top = jnp.full((2 * rows, 1), -jnp.inf, F32)
    total = jnp.zeros((2 * rows, 1), F32)
    acc = jnp.zeros((2 * rows, 2 * HEAD), F32)
    steps = [
        (ref, at) for ref in (mine_ref, other_ref) for at in range(0, ref.shape[0], KEY_STEP)
    ]
    for ref, at in steps:
        block = ref[at : at + KEY_STEP, :]
        scores = lax.dot_general(wide, block, (((1,), (1,)), ((), ())), preferred_element_type=F32)
        new_top = jnp.maximum(top, jnp.max(scores, axis=1, keepdims=True))
        factor = jnp.exp(top - new_top)
        raw = jnp.exp(scores - new_top)
        total = total * factor + jnp.sum(raw, axis=1, keepdims=True)
        acc = acc * factor + jnp.dot(raw.astype(BF16), block, preferred_element_type=F32)
        top = new_top
    done = acc / total
    first = pltpu.roll(done[:rows], HEAD, 1)
    out_ref[...] = jnp.where(lanes < HEAD, first, done[rows:]).astype(BF16)


def attend(query_turned, mine, other):
    rows = query_turned.shape[0]
    keys = mine.shape[0] + other.shape[0]
    return pl.pallas_call(
        attend_body,
        out_shape=jax.ShapeDtypeStruct(query_turned.shape, BF16),
        compiler_params=pltpu.CompilerParams(vmem_limit_bytes=48 * 1024 * 1024),
        cost_estimate=pl.CostEstimate(
            flops=16 * rows * keys * HEAD,
            bytes_accessed=keys * 4 * HEAD,
            transcendentals=2 * rows * keys,
        ),
        name="attend",
    )(query_turned, mine, other)


def route_body(ids_ref, rows_ref, out_ref, slot_ref):
    blocks, cap, _ = out_ref.shape
    count = rows_ref.shape[0]
    lane = lax.broadcasted_iota(jnp.int32, (count, blocks), 1)
    ids = [
        jnp.transpose(jnp.broadcast_to(ids_ref[k : k + 1, :], (8, count)))[:, 0:1] for k in range(2)
    ]
    marks = [(lane == ids[k]).astype(F32) for k in range(2)]
    down = lax.broadcasted_iota(jnp.int32, (count, count), 0)
    across = lax.broadcasted_iota(jnp.int32, (count, count), 1)
    below = (across < down).astype(BF16)
    earlier = jnp.dot(below, (marks[0] + marks[1]).astype(BF16), preferred_element_type=F32)
    places = [
        jnp.sum(earlier * marks[0], axis=1, keepdims=True),
        jnp.sum((earlier + marks[0]) * marks[1], axis=1, keepdims=True),
    ]
    slots = [ids[k] * cap + places[k].astype(jnp.int32) for k in range(2)]
    slot_ref[...] = jnp.concatenate(slots, axis=1)
    slot = lax.broadcasted_iota(jnp.int32, (count, blocks * cap), 1)
    pick = ((slot == slots[0]) | (slot == slots[1])).astype(BF16)
    placed = lax.dot_general(
        pick, rows_ref[...], (((0,), (0,)), ((), ())), preferred_element_type=F32
    )
    for k in range(blocks):
        out_ref[k] = placed[k * cap : (k + 1) * cap, :].astype(BF16)


def mix_body(k_rows, base, joined, index_ref, *refs):
    if joined:
        pieces, refs = [refs[0].at[q] for q in range(SIDE)], refs[1:]
        outs = [refs[-1].at[index_ref[2 * SIDE + r]] for r in range(SIDE)]
    else:
        pieces, outs, refs = refs[:SIDE], refs[-SIDE:], refs[SIDE:]
    weights, gain_ref = refs[:SIDE], refs[SIDE]
    rows = pieces[0].shape[0]
    scaled = [
        (pieces[q][...].astype(F32) * gain_ref[pl.ds(index_ref[SIDE + q], 1), :]).astype(BF16)
        for q in range(SIDE)
    ]
    for r in range(SIDE):
        total = jnp.zeros((rows, weights[r].shape[1]), F32)
        for q in range(SIDE):
            block = weights[r][pl.ds(pl.multiple_of(base + index_ref[q] * k_rows, 128), k_rows), :]
            total += jnp.dot(scaled[q], block, preferred_element_type=F32)
        outs[r][:rows, :] = total.astype(BF16)
    squares = jnp.zeros((rows, k_rows), F32)
    for q in range(SIDE):
        values = pieces[q][...].astype(F32)
        squares += values * values
    high = squares.astype(BF16)
    low = (squares - high.astype(F32)).astype(BF16)
    ones = jnp.ones((8, k_rows), BF16)
    sums = jnp.zeros((8, rows), F32)
    for part in (high, low):
        sums += lax.dot_general(ones, part, (((1,), (1,)), ((), ())), preferred_element_type=F32)
    width = outs[0].shape[1]
    count = -(-rows // width)
    if count * width > rows:
        sums = jnp.concatenate([sums, jnp.zeros((8, count * width - rows), F32)], axis=1)
    line = lax.broadcasted_iota(jnp.int32, (STAT_ROWS, width), 0)
    block = jnp.zeros((STAT_ROWS, width), F32)
    for j in range(count):
        value = sums[0:1, j * width : (j + 1) * width]
        high = value.astype(BF16).astype(F32)
        block = jnp.where(line == j, high, block)
        block = jnp.where(line == count + j, value - high, block)
    for r in range(SIDE):
        outs[r][rows:, :] = block.astype(BF16)


def mix(pieces, weights, base, gains, indices):
    joined = not isinstance(pieces, list)
    rows, k_rows = pieces[0].shape
    width = weights[0].shape[1]
    vmem = pl.BlockSpec(memory_space=pltpu.VMEM)
    shape = (rows + STAT_ROWS, width)
    given = [pieces] if joined else pieces
    return pl.pallas_call(
        functools.partial(mix_body, k_rows, base, joined),
        out_shape=jax.ShapeDtypeStruct((SIDE,) + shape, BF16)
        if joined
        else [jax.ShapeDtypeStruct(shape, BF16)] * SIDE,
        in_specs=[pl.BlockSpec(memory_space=pltpu.SMEM)] + [vmem] * (len(given) + SIDE + 1),
        out_specs=vmem if joined else [vmem] * SIDE,
        compiler_params=pltpu.CompilerParams(vmem_limit_bytes=48 * 1024 * 1024),
        cost_estimate=pl.CostEstimate(
            flops=2 * SIDE * SIDE * rows * k_rows * width,
            bytes_accessed=SIDE * rows * (k_rows + width) * 2,
            transcendentals=0,
        ),
    )(jnp.concatenate(indices), *given, *weights, gains)


def hidden_body(features, in_ref, out_ref):
    rows = out_ref.shape[1]
    hid = out_ref.shape[2]
    width = 2 * hid
    count = -(-rows // width)
    stats = sum(in_ref[k, rows:, :].astype(F32) for k in range(SIDE))
    for j in range(count):
        first, last = j * width, min(rows, (j + 1) * width)
        line = stats[j : j + 1, :] + stats[count + j : count + j + 1, :]
        scale = lax.rsqrt(line / features + EPS)
        column = jnp.transpose(jnp.broadcast_to(scale, (8, width)))[: last - first, 0:1]
        sums = sum(in_ref[k, first:last, :].astype(F32) for k in range(SIDE))
        gate = sums[:, :hid] * column
        up = sums[:, hid:] * column
        result = (gate / (1.0 + jnp.exp(-gate)) * up).astype(BF16)
        for k in range(SIDE):
            out_ref[k, first:last, :] = result


def second_body(index_ref, gathered, *refs):
    weights, out_ref = refs[:SIDE], refs[-1]
    hid = gathered.shape[2]
    wide = jnp.concatenate([gathered[k] for k in range(SIDE)], axis=1)
    for r in range(SIDE):
        out_ref[index_ref[r]] = jnp.dot(
            wide, weights[r][: SIDE * hid, :], preferred_element_type=F32
        ).astype(BF16)


def read_stat(rows, count, size):
    whole = rows.astype(F32)
    return jnp.sum(whole[:, :count] + whole[:, count : 2 * count], axis=0).reshape(-1)[:size]


def send_back(parts, axis):
    return [parts[0]] + [shift(parts[r], axis, SIDE - r) for r in range(1, SIDE)]


def copies_to(array, axis):
    wide = jnp.broadcast_to(array[None], (SIDE,) + array.shape)
    return swap(wide, axis)


def swap(array, axis):
    return lax.all_to_all(array, axis, 0, 0, tiled=True)


def shift(array, axis, by):
    size = lax.axis_size(axis)
    return lax.ppermute(array, axis, [(k, (k + by) % size) for k in range(size)])


def keys_everywhere(mine):
    size = lax.axis_size("z")
    for by in (size // 4, size // 2, size // 8, size // 16):
        came = shift(mine, "z", by)
        mine = jnp.concatenate([mine, came], axis=0)
    return mine, shift(mine, "c", 1)


def deal(chunk_for, axis):
    place = lax.axis_index(axis)
    landed = [chunk_for(place)]
    for by in range(1, SIDE):
        landed.append(shift(chunk_for((place + by) % SIDE), axis, by))
    return landed


def forward(
    queries,
    key_rows,
    values,
    query_gain,
    key_gain,
    mix_gain,
    out_weight,
    expert_input,
    expert_gain,
    route_ids,
    route_weights,
    expert_gate,
    expert_up,
    expert_down,
):
    length = queries.shape[0]
    experts_count = lax.axis_size(EP)
    place_x = lax.axis_index("x")
    place_y = lax.axis_index("y")
    slot_total = experts_count * CAP
    features = expert_gain.shape[0]
    piece = expert_input.shape[1]
    hid = expert_gate.shape[2]

    tables = turn_tables(lax.axis_index(EP) * length, length)
    query_turned, own_rows = turn(
        queries, jnp.concatenate([key_rows, values], axis=1), query_gain, key_gain, tables
    )
    mine, other = keys_everywhere(own_rows)

    outgoing, slot_index = pl.pallas_call(
        route_body,
        out_shape=[
            jax.ShapeDtypeStruct((experts_count, CAP, piece), BF16),
            jax.ShapeDtypeStruct((length, 2), jnp.int32),
        ],
        name="route",
    )(route_ids.T, expert_input)
    arrived = swap(outgoing, EP).reshape(slot_total, piece)

    gate_view = expert_gate.reshape(SIDE, SIDE, piece, hid)
    up_view = expert_up.reshape(SIDE, SIDE, piece, hid)

    def first_chunk(k):
        pair = [lax.dynamic_index_in_dim(w, k, 1, keepdims=False) for w in (gate_view, up_view)]
        return jnp.concatenate(pair, axis=2).reshape(SIDE * piece, 2 * hid)

    def second_chunk(k):
        down = lax.dynamic_slice_in_dim(expert_down[0], k * SIDE * hid, SIDE * hid, 0)
        out = lax.dynamic_slice_in_dim(out_weight, k * SIDE * 2 * HEAD, SIDE * 2 * HEAD, 0)
        return jnp.concatenate([down, out], axis=0)

    first_weights = deal(first_chunk, "x")
    second_weights = deal(second_chunk, "y")

    ahead = jnp.arange(SIDE, dtype=jnp.int32)
    from_y = (place_y - ahead) % SIDE
    from_x = (place_x - ahead) % SIDE
    partial = mix(
        copies_to(arrived, "y"),
        first_weights,
        0,
        expert_gain.reshape(SIDE * SIDE, piece),
        (ahead, ahead * SIDE + place_x, from_x),
    )
    sums = swap(partial, "x")
    hidden = pl.pallas_call(
        functools.partial(hidden_body, features),
        out_shape=jax.ShapeDtypeStruct((SIDE, slot_total, hid), BF16),
        compiler_params=pltpu.CompilerParams(vmem_limit_bytes=48 * 1024 * 1024),
        name="hidden",
    )(sums)

    hidden_all = swap(hidden, "x")
    vmem = pl.BlockSpec(memory_space=pltpu.VMEM)
    expert_partial = pl.pallas_call(
        second_body,
        out_shape=jax.ShapeDtypeStruct((SIDE, slot_total, piece), BF16),
        in_specs=[pl.BlockSpec(memory_space=pltpu.SMEM)] + [vmem] * (1 + SIDE),
        out_specs=vmem,
        compiler_params=pltpu.CompilerParams(vmem_limit_bytes=48 * 1024 * 1024),
        name="second",
    )(from_y, hidden_all, *second_weights)
    landed = swap(expert_partial, "y")
    expert_out = jnp.sum(landed.astype(F32), axis=0).astype(BF16)
    expert_out = expert_out.reshape(experts_count, CAP, piece)

    heads_out = attend(query_turned, mine, other)
    heads = [heads_out, shift(heads_out, "x", 1)]
    heads += [shift(heads_out, "x", by) for by in range(2, SIDE)]
    mix_partial = mix(
        heads,
        second_weights,
        SIDE * hid,
        mix_gain.reshape(SIDE * SIDE, 2 * HEAD),
        (from_x, place_y * SIDE + from_x),
    )
    parts = send_back(mix_partial, "y")
    mix_sum = sum(part[:length].astype(F32) for part in parts)
    mix_square_sum = read_stat(jnp.stack([part[length:] for part in parts]), 1, length)
    mix_scale = lax.rsqrt(mix_square_sum / mix_gain.shape[0] + EPS)
    attended = (mix_sum * mix_scale[:, None]).astype(BF16)

    returned = swap(expert_out, EP).reshape(slot_total, piece)
    slots = jnp.arange(slot_total, dtype=jnp.int32)[None, :]
    first = jnp.dot(
        (slot_index[:, :1] == slots).astype(BF16), returned, preferred_element_type=F32
    )
    second = jnp.dot(
        (slot_index[:, 1:] == slots).astype(BF16), returned, preferred_element_type=F32
    )
    expert_mix = (first * route_weights[:, :1] + second * route_weights[:, 1:]).astype(BF16)
    return (attended, expert_mix)


def solution(mesh):
    torus = Mesh(mesh.devices.reshape(-1, 2, SIDE, SIDE), ("z", "c", "y", "x"))
    return jax.shard_map(
        forward,
        mesh=torus,
        in_specs=(
            P(EP, TP),
            P(EP, TP),
            P(EP, TP),
            P(),
            P(),
            P(),
            P(None, TP),
            P(EP, TP),
            P(),
            P(EP, None),
            P(EP, None),
            P(EP, None, TP),
            P(EP, None, TP),
            P(EP, None, TP),
        ),
        out_specs=(P(EP, TP), P(EP, TP)),
        check_vma=False,
    )
```
